32 devices in a mesh: sp: 8 (over z, x), tp: 4 (over y, core).
Axes of the slice: x: 2, y: 2, z: 4, core: 2. Of those that a mesh axis runs over, the one named last changes fastest.
Arguments:
- query_main: bfloat16 [1024, 2048], P('sp', 'tp'), may hold values from -6 to 6
- query_rotary: bfloat16 [1024, 1024], P('sp', 'tp'), may hold values from -7 to 7
- latent: bfloat16 [1024, 512], P('sp'), may hold values from -8 to 8
- key_rotary: bfloat16 [1024, 64], P('sp'), may hold values from -8 to 8
- key_weight: bfloat16 [512, 2048], P(None, 'tp'), may hold values from -0.25 to 0.25
- value_weight: bfloat16 [512, 2048], P(None, 'tp'), may hold values from -0.25 to 0.25
- head_output: bfloat16 [1024, 2048], P('sp', 'tp'), may hold values from -2 to 2
- output_grad: bfloat16 [1024, 2048], P('sp', 'tp'), may hold values from -40 to 40
- row_logsum: float32 [16, 1024], P('tp', 'sp'), may hold values from 3 to 16, as said below
Outputs:
- grad_query_main: float32 [1024, 2048], P('sp', 'tp')
- grad_query_rotary: float32 [1024, 1024], P('sp', 'tp')
- grad_latent: float32 [1024, 512], P('sp')
- grad_key_rotary: float32 [1024, 64], P('sp')
- grad_key_weight: float32 [512, 2048], P('sp', 'tp')
The draws below stay inside these ranges and needn't reach their ends.
Inputs may be any that keep to these rules, and one draw needn't show every extreme that they name: With p the place of token i in its sequence and q = i % 128, row_logsum[h, i] minus the logarithm of (p + 1 + 54 (q + 1)) lies between -0.3 and 1.5.
All inputs are finite; a program needn't handle non-finite values.
Results may differ from the reference program's by a relative error of at most 0.003.
The reference program's roundings to bfloat16 on the way (of `query_latent`, `grad_rows`, `weights_low`, `dscores_low` and `mixed_low`) count: a program that leaves them out, or rounds other values in their place, can miss the bound.
Values may be sent and summed in bfloat16 or wider, within the bound.
A program may use at most 64 MiB of HBM per device.

```python
import math
import jax
import jax.numpy as jnp
from jax import lax

TOK_DEV = 128
HEADS = 16
KDIM = 128
RDIM = 64
VDIM = 128
LATENT = 512
SPAN = 8
LEAD = 2
SEQS = 2
TOKENS = 1024
N_SP = 8


own_mass = 54.0


def block_signs(key):
    picks = jax.random.randint(jax.random.fold_in(key, 7), (TOKENS // TOK_DEV, RDIM), 0, 2)
    table = picks.astype(jnp.float32) * 2.0 - 1.0
    return table[jnp.arange(TOKENS) // TOK_DEV]


def noise_field(key, shape):
    return jnp.clip(jax.random.normal(key, shape, jnp.float32), -6.0, 6.0)


def draw_query_rotary(key, part):
    signs = block_signs(key)
    noise = noise_field(jax.random.fold_in(key, 11), (TOKENS, HEADS, RDIM))
    return (noise + signs[:, None, :]).reshape(TOKENS, HEADS * RDIM).astype(jnp.bfloat16)


def draw_key_rotary(key, part):
    signs = block_signs(key)
    noise = noise_field(jax.random.fold_in(key, 13), (TOKENS, RDIM))
    strength = 4.0 * (KDIM + RDIM) ** 0.5 / RDIM
    return (noise + strength * signs).astype(jnp.bfloat16)


def draw_row_logsum(key, part):
    token = jnp.arange(TOKENS)
    device = token // TOK_DEV
    sequence = (device + LEAD) // SPAN
    first_device = jnp.maximum(sequence * SPAN - LEAD, 0)
    place = (token - first_device * TOK_DEV + 1).astype(jnp.float32)
    inside = (token % TOK_DEV + 1).astype(jnp.float32)
    total = place + own_mass * inside
    offset = jax.random.uniform(key, (HEADS, TOKENS), jnp.float32, 0.2, 1.2)
    return jnp.log(total)[None, :] + offset


def with_spikes(drawn, own_key, source, target, parts, factor):
    def block_of(axis_at):
        return (jnp.arange(drawn.shape[axis_at]) // (drawn.shape[axis_at] // parts)).reshape((-1,) + (1,) * (drawn.ndim - 1 - axis_at))

    near = jax.random.permutation(own_key, parts)[block_of(target)]
    second = (block_of(target) + parts // 2) % parts
    return jnp.where((block_of(source) == near) | (block_of(source) == second), factor * drawn, drawn)


def levels(key, shape, split, smallest, top_value):
    gain = 1.0
    for axis_at, parts in split:
        heights = jax.random.uniform(jax.random.fold_in(jax.random.fold_in(key, 6), axis_at), (parts,), jnp.float32, smallest / len(split), top_value / len(split))
        gain = gain * jnp.repeat(jnp.exp(heights), shape[axis_at] // parts).reshape((-1,) + (1,) * (len(shape) - 1 - axis_at))
    return gain


def centred(stream_key, extent, scale, bound, pieces=(), held_as=jnp.bfloat16):
    entries = jax.random.normal(stream_key, extent, jnp.float32) * scale
    if len(pieces) > 0:
        entries = levels(stream_key, extent, pieces, -0.22, 0.18) * entries
    return jnp.clip(entries, min=-bound, max=bound).astype(held_as)


def noise_with(own_key, shape, spread, most, split, heavy, held_as=jnp.bfloat16):
    entries = spread * jax.random.normal(own_key, shape, jnp.float32)
    if split:
        entries = entries * levels(own_key, shape, split, -0.22, 0.18)
    return jnp.clip(with_spikes(entries, jax.random.fold_in(own_key, 3), *heavy), -most, most).astype(held_as)


def setup_inputs(seed: int = 0) -> dict:
    seeds = jax.random.split(jax.random.key(seed), 10)
    query_main = centred(seeds[0], (TOKENS, HEADS * KDIM), 1.0, 6.0, ((0, 8), (1, 4)))
    query_rotary = draw_query_rotary(jax.random.fold_in(seeds[9], 71), 0)
    latent = noise_with(seeds[2], (TOKENS, LATENT), 1.0, 8.0, ((0, 8),), (0, 1, 8, 2.0))
    key_rotary = draw_key_rotary(jax.random.fold_in(seeds[9], 71), 0)
    key_weight = centred(seeds[4], (LATENT, HEADS * KDIM), LATENT ** -0.5, 0.25, ((1, 4),))
    value_weight = centred(seeds[5], (LATENT, HEADS * VDIM), LATENT ** -0.5, 0.25, ((1, 4),))
    head_output = centred(seeds[6], (TOKENS, HEADS * VDIM), 0.3, 2.0, ((0, 8), (1, 4)))
    output_grad = noise_with(seeds[7], (TOKENS, HEADS * VDIM), 6.0, 40.0, ((0, 8), (1, 4)), (0, 1, 8, 2.0))
    row_logsum = draw_row_logsum(jax.random.fold_in(seeds[9], 71), 0)
    return {"query_main": query_main, "query_rotary": query_rotary, "latent": latent, "key_rotary": key_rotary, "key_weight": key_weight, "value_weight": value_weight, "head_output": head_output, "output_grad": output_grad, "row_logsum": row_logsum}


def sequence_grads(lat_seq, rot_seq, query_latent, grad_rows, rot_query, row_logs, row_terms, factor, width):
    wide = jnp.float32
    blocks = lat_seq.shape[0] // width
    heads = query_latent.shape[1]
    lat_all = lat_seq.astype(wide)
    rot_all = rot_seq.astype(wide)
    qlat_all = query_latent.astype(wide)
    grows_all = grad_rows.astype(wide)
    qrot_all = rot_query.astype(wide)

    def query_block(carry, query_index):
        acc_lat, acc_rot = carry
        query_start = (query_index * width).astype(jnp.int32)
        qlat = lax.dynamic_slice_in_dim(qlat_all, query_start, width, 0)
        grows = lax.dynamic_slice_in_dim(grows_all, query_start, width, 0)
        qrot = lax.dynamic_slice_in_dim(qrot_all, query_start, width, 0)
        logs = lax.dynamic_slice_in_dim(row_logs, query_start, width, 0)
        terms = lax.dynamic_slice_in_dim(row_terms, query_start, width, 0)
        query_place = query_start + jnp.arange(width, dtype=jnp.int32)

        def key_block(key_index, inner):
            def visit(state):
                mixed_sum, rot_sum, acc_lat, acc_rot = state
                key_start = (key_index * width).astype(jnp.int32)
                lat_block = lax.dynamic_slice_in_dim(lat_all, key_start, width, 0)
                rot_block = lax.dynamic_slice_in_dim(rot_all, key_start, width, 0)
                key_place = key_start + jnp.arange(width, dtype=jnp.int32)
                seen = key_place[None, :] <= query_place[:, None]
                scores = jnp.einsum("thl,kl->thk", qlat, lat_block) + jnp.einsum("thr,kr->thk", qrot, rot_block)
                weights = jnp.where(seen[:, None, :], jnp.exp(factor * scores - logs[:, :, None]), 0.0)
                slopes = jnp.einsum("thl,kl->thk", grows, lat_block)
                dscores = weights * (slopes - terms[:, :, None])
                weights_low = lax.optimization_barrier(weights.astype(jnp.bfloat16)).astype(wide)
                dscores_low = lax.optimization_barrier(dscores.astype(jnp.bfloat16)).astype(wide)
                mixed_sum = mixed_sum + jnp.einsum("thk,kl->thl", dscores_low, lat_block)
                rot_sum = rot_sum + jnp.einsum("thk,kr->thr", dscores_low, rot_block)
                part_lat = factor * jnp.einsum("thk,thl->kl", dscores_low, qlat) + jnp.einsum("thk,thl->kl", weights_low, grows)
                part_rot = factor * jnp.einsum("thk,thr->kr", dscores_low, qrot)
                old_lat = lax.dynamic_slice_in_dim(acc_lat, key_start, width, 0)
                old_rot = lax.dynamic_slice_in_dim(acc_rot, key_start, width, 0)
                acc_lat = lax.dynamic_update_slice_in_dim(acc_lat, old_lat + part_lat, key_start, 0)
                acc_rot = lax.dynamic_update_slice_in_dim(acc_rot, old_rot + part_rot, key_start, 0)
                return mixed_sum, rot_sum, acc_lat, acc_rot

            def keep(state):
                return state

            return lax.cond(key_index <= query_index, visit, keep, inner)

        start_state = (jnp.zeros((width, heads, lat_all.shape[1]), wide), jnp.zeros((width, heads, rot_all.shape[1]), wide), acc_lat, acc_rot)
        mixed_sum, rot_sum, acc_lat, acc_rot = lax.fori_loop(0, blocks, key_block, start_state)
        return (acc_lat, acc_rot), (mixed_sum, rot_sum)

    start = (jnp.zeros(lat_seq.shape, wide), jnp.zeros(rot_seq.shape, wide))
    (acc_lat, acc_rot), (mixed_parts, rot_parts) = lax.scan(query_block, start, jnp.arange(blocks, dtype=jnp.int32))
    mixed = mixed_parts.reshape(lat_seq.shape[0], heads, lat_seq.shape[1])
    rot_sum = rot_parts.reshape(lat_seq.shape[0], heads, rot_seq.shape[1])
    return mixed, rot_sum, acc_lat, acc_rot


def reference(query_main, query_rotary, latent, key_rotary, key_weight, value_weight, head_output, output_grad, row_logsum):
    wide = jnp.float32
    factor = (KDIM + RDIM) ** -0.5
    count = latent.shape[0]
    width = math.gcd(LEAD * TOK_DEV, 512)
    main_query = query_main.reshape(count, HEADS, KDIM).astype(wide)
    rot_query = query_rotary.reshape(count, HEADS, RDIM)
    key_proj = key_weight.reshape(LATENT, HEADS, KDIM).astype(wide)
    value_proj = value_weight.reshape(LATENT, HEADS, VDIM).astype(wide)
    grad_heads = output_grad.reshape(count, HEADS, VDIM).astype(wide)
    query_latent = jnp.einsum("thd,lhd->thl", main_query, key_proj).astype(jnp.bfloat16)
    grad_rows = jnp.einsum("thd,lhd->thl", grad_heads, value_proj).astype(jnp.bfloat16)
    row_terms = jnp.sum(head_output.reshape(count, HEADS, VDIM).astype(wide) * grad_heads, axis=2)
    row_logs = row_logsum.T.astype(wide)
    mixed_list, rot_list, lat_list, key_rot_list = [], [], [], []
    for sequence in range(SEQS):
        first = max(sequence * SPAN - LEAD, 0) * TOK_DEV
        last = min((sequence + 1) * SPAN - LEAD, N_SP) * TOK_DEV
        mixed, rot_sum, acc_lat, acc_rot = sequence_grads(
            latent[first:last], key_rotary[first:last], query_latent[first:last], grad_rows[first:last],
            rot_query[first:last], row_logs[first:last], row_terms[first:last], factor, width)
        mixed_list.append(mixed)
        rot_list.append(rot_sum)
        lat_list.append(acc_lat)
        key_rot_list.append(acc_rot)
    mixed = jnp.concatenate(mixed_list, axis=0)
    rot_sum = jnp.concatenate(rot_list, axis=0)
    grad_latent = jnp.concatenate(lat_list, axis=0)
    grad_key_rotary = jnp.concatenate(key_rot_list, axis=0)
    mixed_low = lax.optimization_barrier(mixed.astype(jnp.bfloat16)).astype(wide)
    grad_query_main = (factor * jnp.einsum("thl,lhd->thd", mixed_low, key_proj)).reshape(count, HEADS * KDIM)
    grad_query_rotary = (factor * rot_sum).reshape(count, HEADS * RDIM)
    grad_key_weight = (factor * jnp.einsum("thl,thd->lhd", mixed_low, main_query)).reshape(LATENT, HEADS * KDIM)
    return (grad_query_main, grad_query_rotary, grad_latent, grad_key_rotary, grad_key_weight)
```

```python
import functools

import jax
import jax.numpy as jnp
from jax import lax
from jax.experimental import pallas as pl
from jax.experimental.pallas import tpu as pltpu
from jax.sharding import PartitionSpec as P

SEQ_DEVICES = 32
MESH = pl.DeviceIdType.MESH
F32 = jnp.float32
BF16 = jnp.bfloat16


def dot(a, b, ca, cb, precision=None):
    return lax.dot_general(
        a, b, (((ca,), (cb,)), ((), ())), preferred_element_type=F32, precision=precision
    )


def kernel(
    dims,
    qm, qr, lat, rot, kw, vw, ho, og, logs,
    o_main, o_rot, o_lat, o_krot, o_kw,
    lat_buf, rot_buf, ql, gr, qrp, mixed, rsum, gpart, obuf, kwst, kwrecv, fin_s, fin_r,
    ksend, krecv, fsend, frecv, finsend, finrecv, agsend, agrecv, kwsend, kwrecvs,
    *halving,
):
    n_sp, n_tp, heads, factor = dims
    stages = n_tp.bit_length() - 1
    half_s, half_r = halving[:stages], halving[stages : 2 * stages]
    half_ss, half_rs = halving[2 * stages : 3 * stages], halving[3 * stages :]
    span = min(SEQ_DEVICES, n_sp)
    lead = span // 4
    tok, width = lat.shape
    rdim = rot.shape[1]
    kdim = kw.shape[1] // heads
    vdim = vw.shape[1] // heads
    sp = lax.axis_index("sp")
    tp = lax.axis_index("tp")
    seq = (sp + lead) // span
    first = jnp.maximum(seq * span - lead, 0)
    last = jnp.minimum((seq + 1) * span - lead, n_sp)
    before = sp - first
    after = last - 1 - sp
    low = tp % 2
    pair = tp + 1 - 2 * low
    half = tok // 2

    barrier = pltpu.get_barrier_semaphore()

    @pl.loop(1, n_sp)
    def _(d):
        pl.semaphore_signal(
            barrier, inc=1, device_id={"sp": (sp + d) % n_sp}, device_id_type=MESH
        )

    for t in range(1, n_tp):
        pl.semaphore_signal(
            barrier, inc=1, device_id={"tp": (tp + t) % n_tp}, device_id_type=MESH
        )
    pl.semaphore_wait(barrier, n_sp - 1 + n_tp - 1)

    mine = pl.ds(pl.multiple_of(low * half, half), half)
    theirs = pl.ds(pl.multiple_of((1 - low) * half, half), half)

    def key_copies(i):
        return [
            pltpu.make_async_remote_copy(
                src_ref=src.at[mine], dst_ref=dst.at[i, mine],
                send_sem=ksend.at[i, n], recv_sem=krecv.at[i, n],
                device_id={"sp": sp + i}, device_id_type=MESH,
            )
            for n, (src, dst) in enumerate(((lat, lat_buf), (rot, rot_buf)))
        ]

    def forward_copies(i, rows):
        return [
            pltpu.make_async_remote_copy(
                src_ref=buf.at[i, rows], dst_ref=buf.at[i, rows],
                send_sem=fsend.at[i, n], recv_sem=frecv.at[i, n],
                device_id={"tp": pair}, device_id_type=MESH,
            )
            for n, buf in enumerate((lat_buf, rot_buf))
        ]

    @pl.loop(1, after + 1)
    def _(i):
        for c in key_copies(i):
            c.start()

    lat_buf[0] = lat[...]
    rot_buf[0] = rot[...]
    terms_parts = []
    for h in range(heads):
        rows = slice(h * tok, (h + 1) * tok)
        kcols = slice(h * kdim, (h + 1) * kdim)
        vcols = slice(h * vdim, (h + 1) * vdim)
        ql[rows] = dot(qm[:, kcols], kw[:, kcols], 1, 1).astype(BF16)
        gr[rows] = dot(og[:, vcols], vw[:, vcols], 1, 1).astype(BF16)
        qrp[rows] = jnp.concatenate(
            [qr[:, h * rdim : (h + 1) * rdim], jnp.zeros((tok, qrp.shape[1] - rdim), BF16)], axis=1
        )
        prod = ho[:, vcols].astype(F32) * og[:, vcols].astype(F32)
        terms_parts.append(
            dot(jnp.ones((8, vdim), F32), prod, 1, 1, lax.Precision.HIGHEST)[0:1]
        )
    terms = jnp.concatenate(terms_parts, axis=1)
    row_logs = jnp.concatenate([logs[h : h + 1, :] for h in range(heads)], axis=1)
    mixed[...] = jnp.zeros_like(mixed)
    rsum[...] = jnp.zeros_like(rsum)

    def level_offset(level):
        off = 0
        for b in range(level):
            off = off + ((tp // (1 << b)) % 2) * (tok >> (b + 1))
        return off

    def half_copy(s, i):
        bit = (tp // (1 << s)) % 2
        return pltpu.make_async_remote_copy(
            src_ref=half_s[s].at[i], dst_ref=half_r[s].at[i],
            send_sem=half_ss[s].at[i], recv_sem=half_rs[s].at[i],
            device_id={"tp": tp + (1 - 2 * bit) * (1 << s)}, device_id_type=MESH,
        )

    def send_half(s, i):
        size = tok >> (s + 1)
        bit = (tp // (1 << s)) % 2
        start = pl.multiple_of(level_offset(s) + (1 - bit) * size, size)
        half_s[s][i] = gpart[i, pl.ds(start, size), :].astype(BF16)
        half_copy(s, i).start()

    def fin_copy(i):
        return pltpu.make_async_remote_copy(
            src_ref=fin_s.at[i], dst_ref=fin_r.at[i],
            send_sem=finsend.at[i], recv_sem=finrecv.at[i],
            device_id={"sp": sp - i}, device_id_type=MESH,
        )

    def arrive(i):
        for c in key_copies(i):
            c.wait_recv()
        for c in forward_copies(i, mine):
            c.start()

    quarter = tok >> stages
    my_rows = pl.ds(pl.multiple_of(level_offset(stages), quarter), quarter)

    def attend(i):
        @pl.when(i < before)
        def _():
            arrive(i + 1)

        @pl.when(i > 0)
        def _():
            for c in forward_copies(i, theirs):
                c.wait_recv()

        lt = lat_buf[i]
        rt = rot_buf[i]
        scores = dot(lt, ql[...], 1, 1) + dot(rt, qrp[:, :rdim], 1, 1)
        weights = jnp.exp(factor * scores - row_logs)
        key_at = lax.broadcasted_iota(jnp.int32, weights.shape, 0)
        query_at = lax.broadcasted_iota(jnp.int32, weights.shape, 1) % tok
        weights = jnp.where((key_at <= query_at) | (i > 0), weights, 0.0)
        slopes = dot(lt, gr[...], 1, 1)
        dscores = weights * (slopes - terms)
        wl = weights.astype(BF16)
        dl = dscores.astype(BF16)
        gpart[i, :, :width] = factor * dot(dl, ql[...], 1, 0) + dot(wl, gr[...], 1, 0)
        gpart[i, :, width:] = factor * dot(dl, qrp[...], 1, 0)
        send_half(0, i)
        mixed[...] += dot(dl, lt, 0, 0)
        rsum[...] += dot(dl, rt, 0, 0)

    @pl.loop(0, before + 1 + stages)
    def _(it):
        @pl.when(it <= before)
        def _():
            attend(it)

        for s in range(1, stages + 1):
            i = it - s

            @pl.when((i >= 0) & (i <= before))
            def _():
                half_copy(s - 1, i).wait_recv()
                size = tok >> s
                rows = pl.ds(pl.multiple_of(level_offset(s), size), size)
                gpart[i, rows, :] += half_r[s - 1][i].astype(F32)
                if s < stages:
                    send_half(s, i)
                else:

                    @pl.when(i > 0)
                    def _():
                        fin_s[i] = gpart[i, rows, :].astype(BF16)
                        fin_copy(i).start()

    part = o_kw.shape[0]

    def kw_copy(d):
        dest = (sp + d) % n_sp
        return pltpu.make_async_remote_copy(
            src_ref=kwst.at[dest], dst_ref=kwrecv.at[n_sp - d],
            send_sem=kwsend.at[d], recv_sem=kwrecvs.at[n_sp - d],
            device_id={"sp": dest}, device_id_type=MESH,
        )

    def kw_landing(d):
        return pltpu.make_async_remote_copy(
            src_ref=kwst.at[0], dst_ref=kwrecv.at[d],
            send_sem=kwsend.at[d], recv_sem=kwrecvs.at[d],
            device_id={"sp": (sp + d) % n_sp}, device_id_type=MESH,
        )

    low_parts = []
    for h in range(heads):
        rows = slice(h * tok, (h + 1) * tok)
        kcols = slice(h * kdim, (h + 1) * kdim)
        ml = mixed[rows].astype(BF16)
        term = (factor * dot(ml, qm[:, kcols], 0, 0)).astype(BF16)
        for d in range(n_sp):
            kwst[d, :, kcols] = term[d * part : (d + 1) * part]
        low_parts.append(ml)

    @pl.loop(1, n_sp)
    def _(d):
        kw_copy(d).start()

    for h in range(heads):
        rows = slice(h * tok, (h + 1) * tok)
        kcols = slice(h * kdim, (h + 1) * kdim)
        o_main[:, kcols] = factor * dot(low_parts[h], kw[:, kcols], 1, 0)
        o_rot[:, h * rdim : (h + 1) * rdim] = factor * rsum[rows]

    @pl.loop(1, after + 1)
    def _(i):
        pltpu.make_async_remote_copy(
            src_ref=fin_s.at[i], dst_ref=fin_r.at[i],
            send_sem=finsend.at[i], recv_sem=finrecv.at[i],
            device_id={"sp": sp + i}, device_id_type=MESH,
        ).wait_recv()
        gpart[0, my_rows, :] += fin_r[i].astype(F32)

    obuf[my_rows] = gpart[0, my_rows, :]

    def ag_copy(t):
        return pltpu.make_async_remote_copy(
            src_ref=obuf.at[my_rows], dst_ref=obuf.at[my_rows],
            send_sem=agsend.at[t], recv_sem=agrecv.at[n_tp - t],
            device_id={"tp": (tp + t) % n_tp}, device_id_type=MESH,
        )

    for t in range(1, n_tp):
        ag_copy(t).start()

    total = kwst[sp].astype(F32)
    for d in range(1, n_sp):
        kw_landing(d).wait_recv()
        total = total + kwrecv[d].astype(F32)
    o_kw[...] = total

    for t in range(1, n_tp):
        peer = (tp + t) % n_tp
        off = 0
        for b in range(stages):
            off = off + ((peer // (1 << b)) % 2) * (tok >> (b + 1))
        rows = pl.ds(pl.multiple_of(off, quarter), quarter)
        pltpu.make_async_remote_copy(
            src_ref=obuf.at[rows], dst_ref=obuf.at[rows],
            send_sem=agsend.at[t], recv_sem=agrecv.at[t],
            device_id={"tp": peer}, device_id_type=MESH,
        ).wait_recv()
    o_lat[...] = obuf[:, :width]
    o_krot[...] = obuf[:, width : width + rdim]

    @pl.loop(1, after + 1)
    def _(i):
        for c in key_copies(i):
            c.wait_send()

    @pl.loop(0, before + 1)
    def _(i):
        for s in range(stages):
            half_copy(s, i).wait_send()

        @pl.when(i > 0)
        def _():
            for c in forward_copies(i, mine):
                c.wait_send()
            fin_copy(i).wait_send()

    @pl.loop(1, n_sp)
    def _(d):
        kw_copy(d).wait_send()

    for t in range(1, n_tp):
        ag_copy(t).wait_send()


def per_device(mesh_dims, *args):
    n_sp, n_tp = mesh_dims
    qm, qr, lat, rot, kw, vw, ho, og, logs = args
    heads, tok = logs.shape
    width, rdim = lat.shape[1], rot.shape[1]
    factor = (kw.shape[1] // heads + rdim) ** (-0.5)
    span = min(SEQ_DEVICES, n_sp)
    stages = n_tp.bit_length() - 1
    rpad = -(-rdim // 128) * 128
    wide = width + rpad
    quarter = tok >> stages
    part = width // n_sp
    dma = pltpu.SemaphoreType.DMA
    scratch = [
        pltpu.VMEM((span, tok, width), BF16),
        pltpu.VMEM((span, tok, rdim), BF16),
        pltpu.VMEM((heads * tok, width), BF16),
        pltpu.VMEM((heads * tok, width), BF16),
        pltpu.VMEM((heads * tok, rpad), BF16),
        pltpu.VMEM((heads * tok, width), F32),
        pltpu.VMEM((heads * tok, rdim), F32),
        pltpu.VMEM((span, tok, wide), F32),
        pltpu.VMEM((tok, wide), F32),
        pltpu.VMEM((n_sp, part, kw.shape[1]), BF16),
        pltpu.VMEM((n_sp, part, kw.shape[1]), BF16),
        pltpu.VMEM((span, quarter, wide), BF16),
        pltpu.VMEM((span, quarter, wide), BF16),
        dma((span, 2)), dma((span, 2)), dma((span, 2)), dma((span, 2)),
        dma((span,)), dma((span,)), dma((n_tp,)), dma((n_tp,)), dma((n_sp,)), dma((n_sp,)),
    ]
    halves = [pltpu.VMEM((span, tok >> (s + 1), wide), BF16) for s in range(stages)]
    sems = [dma((span,)) for s in range(stages)]
    scratch = scratch + halves + halves + sems + sems
    outs = (
        jax.ShapeDtypeStruct((tok, kw.shape[1]), F32),
        jax.ShapeDtypeStruct((tok, heads * rdim), F32),
        jax.ShapeDtypeStruct((tok, width), F32),
        jax.ShapeDtypeStruct((tok, rdim), F32),
        jax.ShapeDtypeStruct((part, kw.shape[1]), F32),
    )
    vmem = pl.BlockSpec(memory_space=pltpu.VMEM)
    return pl.pallas_call(
        functools.partial(kernel, (n_sp, n_tp, heads, factor)),
        out_shape=outs,
        in_specs=[vmem] * len(args),
        out_specs=[vmem] * len(outs),
        scratch_shapes=scratch,
        compiler_params=pltpu.CompilerParams(collective_id=0, has_side_effects=True),
        name="latent_attention_backward",
    )(*args)


def solution(mesh):
    dims = (mesh.shape["sp"], mesh.shape["tp"])
    return jax.shard_map(
        functools.partial(per_device, dims),
        mesh=mesh,
        in_specs=(
            P("sp", "tp"),
            P("sp", "tp"),
            P("sp", None),
            P("sp", None),
            P(None, "tp"),
            P(None, "tp"),
            P("sp", "tp"),
            P("sp", "tp"),
            P("tp", "sp"),
        ),
        out_specs=(P("sp", "tp"), P("sp", "tp"), P("sp", None), P("sp", None), P("sp", "tp")),
        check_vma=False,
    )
```

```python
import functools
import math

import jax
import jax.numpy as jnp
from jax import lax
from jax.experimental import pallas as pl
from jax.experimental.pallas import tpu as pltpu
from jax.sharding import PartitionSpec as P

SEQ_DEVICES = 32
VMEM_BYTES = 67043328
MESH = pl.DeviceIdType.MESH
F32 = jnp.float32
BF16 = jnp.bfloat16


def dot(a, b, ca, cb, precision=None):
    return lax.dot_general(
        a, b, (((ca,), (cb,)), ((), ())), preferred_element_type=F32, precision=precision
    )


def kernel(
    dims,
    qm_h, qr_h, lat_h, rot_h, kw_h, vw_h, ho_h, og_h, logs_h,
    o_main, o_rot, o_lat, o_krot, o_kw,
    qm, qr, lat, rot, kw, vw, ho, og, logs, insem,
    lat_buf, rot_buf, ql, gr, qrp, mixed, rsum, gpart, obuf, kwst, kwrecv, fin_s, fin_r,
    ksend, krecv, fsend, frecv, finsend, finrecv, agsend, agrecv, kwsend, kwrecvs,
    *halving,
):
    n_sp, n_tp, heads, factor = dims
    stages = n_tp.bit_length() - 1
    half_s, half_r = halving[:stages], halving[stages : 2 * stages]
    half_ss, half_rs = halving[2 * stages : 3 * stages], halving[3 * stages :]
    span = min(SEQ_DEVICES, n_sp)
    lead = span // 4
    tok, width = lat.shape
    rdim = rot.shape[0]
    kdim = kw.shape[1] // heads
    vdim = vw.shape[1] // heads
    loads = [
        pltpu.make_async_copy(src, dst, insem.at[n])
        for n, (src, dst) in enumerate(
            (
                (lat_h, lat), (rot_h, rot), (qm_h, qm), (kw_h, kw), (og_h, og), (vw_h, vw),
                (ho_h, ho), (qr_h, qr), (logs_h, logs),
            )
        )
    ]
    for c in loads:
        c.start()
    sp = lax.axis_index("sp")
    tp = lax.axis_index("tp")
    seq = (sp + lead) // span
    first = jnp.maximum(seq * span - lead, 0)
    last = jnp.minimum((seq + 1) * span - lead, n_sp)
    before = sp - first
    after = last - 1 - sp
    low = tp % 2
    pair = tp + 1 - 2 * low

    barrier = pltpu.get_barrier_semaphore()

    @pl.loop(1, n_sp)
    def _(d):
        pl.semaphore_signal(
            barrier, inc=1, device_id={"sp": (sp + d) % n_sp}, device_id_type=MESH
        )

    for t in range(1, n_tp):
        pl.semaphore_signal(
            barrier, inc=1, device_id={"tp": (tp + t) % n_tp}, device_id_type=MESH
        )
    pl.semaphore_wait(barrier, n_sp - 1 + n_tp - 1)

    def part_of(side, size):
        return pl.ds(pl.multiple_of(side * (size // 2), size // 2), size // 2)

    keys = ((lat, lat_buf, tok), (rot, rot_buf, rdim))

    def key_copies(i):
        return [
            pltpu.make_async_remote_copy(
                src_ref=src.at[part_of(low, size)], dst_ref=dst.at[i, part_of(low, size)],
                send_sem=ksend.at[i, n], recv_sem=krecv.at[i, n],
                device_id={"sp": sp + i}, device_id_type=MESH,
            )
            for n, (src, dst, size) in enumerate(keys)
        ]

    def forward_copies(i, side):
        return [
            pltpu.make_async_remote_copy(
                src_ref=buf.at[i, part_of(side, size)], dst_ref=buf.at[i, part_of(side, size)],
                send_sem=fsend.at[i, n], recv_sem=frecv.at[i, n],
                device_id={"tp": pair}, device_id_type=MESH,
            )
            for n, (_, buf, size) in enumerate(keys)
        ]

    loads[0].wait()
    loads[1].wait()

    @pl.loop(1, after + 1)
    def _(i):
        for c in key_copies(i):
            c.start()

    lat_buf[0] = lat[...]
    rot_buf[0] = rot[...]
    for c in loads[2:]:
        c.wait()
    terms_parts = []
    for h in range(heads):
        rows = slice(h * tok, (h + 1) * tok)
        kcols = slice(h * kdim, (h + 1) * kdim)
        vcols = slice(h * vdim, (h + 1) * vdim)
        ql[rows] = dot(qm[:, kcols], kw[:, kcols], 1, 1).astype(BF16)
        gr[rows] = dot(og[:, vcols], vw[:, vcols], 1, 1).astype(BF16)
        qrp[rows] = jnp.concatenate(
            [qr[:, h * rdim : (h + 1) * rdim], jnp.zeros((tok, qrp.shape[1] - rdim), BF16)], axis=1
        )
        prod = ho[:, vcols].astype(F32) * og[:, vcols].astype(F32)
        terms_parts.append(
            dot(jnp.ones((8, vdim), F32), prod, 1, 1, lax.Precision.HIGHEST)[0:1]
        )
    terms = jnp.concatenate(terms_parts, axis=1)
    row_logs = jnp.concatenate([logs[h : h + 1, :] for h in range(heads)], axis=1)
    mixed[...] = jnp.zeros_like(mixed)
    rsum[...] = jnp.zeros_like(rsum)

    def level_offset(level):
        off = 0
        for b in range(level):
            off = off + ((tp // (1 << b)) % 2) * (tok >> (b + 1))
        return off

    def half_copy(s, i):
        bit = (tp // (1 << s)) % 2
        return pltpu.make_async_remote_copy(
            src_ref=half_s[s].at[i], dst_ref=half_r[s].at[i],
            send_sem=half_ss[s].at[i], recv_sem=half_rs[s].at[i],
            device_id={"tp": tp + (1 - 2 * bit) * (1 << s)}, device_id_type=MESH,
        )

    def send_half(s, i):
        size = tok >> (s + 1)
        bit = (tp // (1 << s)) % 2
        start = pl.multiple_of(level_offset(s) + (1 - bit) * size, size)
        half_s[s][i] = gpart[i, pl.ds(start, size), :].astype(BF16)
        half_copy(s, i).start()

    def fin_copy(i):
        return pltpu.make_async_remote_copy(
            src_ref=fin_s.at[i], dst_ref=fin_r.at[i],
            send_sem=finsend.at[i], recv_sem=finrecv.at[i],
            device_id={"sp": sp - i}, device_id_type=MESH,
        )

    def arrive(i):
        for c in key_copies(i):
            c.wait_recv()
        for c in forward_copies(i, low):
            c.start()

    quarter = tok >> stages
    my_rows = pl.ds(pl.multiple_of(level_offset(stages), quarter), quarter)

    def attend(i):
        @pl.when(i < before)
        def _():
            arrive(i + 1)

        @pl.when(i > 0)
        def _():
            for c in forward_copies(i, 1 - low):
                c.wait_recv()

        lt = lat_buf[i]
        rt = rot_buf[i]
        scores = dot(lt, ql[...], 1, 1) + dot(rt, qrp[:, :rdim], 0, 1)
        weights = jnp.exp(factor * scores - row_logs)
        key_at = lax.broadcasted_iota(jnp.int32, weights.shape, 0)
        query_at = lax.broadcasted_iota(jnp.int32, weights.shape, 1) % tok
        weights = jnp.where((key_at <= query_at) | (i > 0), weights, 0.0)
        slopes = dot(lt, gr[...], 1, 1)
        dscores = weights * (slopes - terms)
        wl = weights.astype(BF16)
        dl = dscores.astype(BF16)
        gpart[i, :, :width] = factor * dot(dl, ql[...], 1, 0) + dot(wl, gr[...], 1, 0)
        gpart[i, :, width:] = factor * dot(dl, qrp[...], 1, 0)
        send_half(0, i)
        mixed[...] += dot(dl, lt, 0, 0)
        rsum[...] += dot(dl, rt, 0, 1)

    @pl.loop(0, before + 1 + stages)
    def _(it):
        @pl.when(it <= before)
        def _():
            attend(it)

        for s in range(1, stages + 1):
            i = it - s

            @pl.when((i >= 0) & (i <= before))
            def _():
                half_copy(s - 1, i).wait_recv()
                size = tok >> s
                rows = pl.ds(pl.multiple_of(level_offset(s), size), size)
                gpart[i, rows, :] += half_r[s - 1][i].astype(F32)
                if s < stages:
                    send_half(s, i)
                else:

                    @pl.when(i > 0)
                    def _():
                        fin_s[i] = gpart[i, rows, :].astype(BF16)
                        fin_copy(i).start()

    part = o_kw.shape[0]

    def kw_copy(d):
        dest = (sp + d) % n_sp
        return pltpu.make_async_remote_copy(
            src_ref=kwst.at[dest], dst_ref=kwrecv.at[n_sp - d],
            send_sem=kwsend.at[d], recv_sem=kwrecvs.at[n_sp - d],
            device_id={"sp": dest}, device_id_type=MESH,
        )

    def kw_landing(d):
        return pltpu.make_async_remote_copy(
            src_ref=kwst.at[0], dst_ref=kwrecv.at[d],
            send_sem=kwsend.at[d], recv_sem=kwrecvs.at[d],
            device_id={"sp": (sp + d) % n_sp}, device_id_type=MESH,
        )

    low_parts = []
    for h in range(heads):
        rows = slice(h * tok, (h + 1) * tok)
        kcols = slice(h * kdim, (h + 1) * kdim)
        ml = mixed[rows].astype(BF16)
        term = (factor * dot(ml, qm[:, kcols], 0, 0)).astype(BF16)
        for d in range(n_sp):
            kwst[d, :, kcols] = term[d * part : (d + 1) * part]
        low_parts.append(ml)

    @pl.loop(1, n_sp)
    def _(d):
        kw_copy(d).start()

    for h in range(heads):
        rows = slice(h * tok, (h + 1) * tok)
        kcols = slice(h * kdim, (h + 1) * kdim)
        o_main[:, kcols] = factor * dot(low_parts[h], kw[:, kcols], 1, 0)
        o_rot[:, h * rdim : (h + 1) * rdim] = factor * rsum[rows]

    @pl.loop(1, after + 1)
    def _(i):
        pltpu.make_async_remote_copy(
            src_ref=fin_s.at[i], dst_ref=fin_r.at[i],
            send_sem=finsend.at[i], recv_sem=finrecv.at[i],
            device_id={"sp": sp + i}, device_id_type=MESH,
        ).wait_recv()
        gpart[0, my_rows, :] += fin_r[i].astype(F32)

    obuf[my_rows] = gpart[0, my_rows, :]

    def ag_copy(t):
        return pltpu.make_async_remote_copy(
            src_ref=obuf.at[my_rows], dst_ref=obuf.at[my_rows],
            send_sem=agsend.at[t], recv_sem=agrecv.at[n_tp - t],
            device_id={"tp": (tp + t) % n_tp}, device_id_type=MESH,
        )

    for t in range(1, n_tp):
        ag_copy(t).start()

    total = kwst[sp].astype(F32)
    for d in range(1, n_sp):
        kw_landing(d).wait_recv()
        total = total + kwrecv[d].astype(F32)
    o_kw[...] = total

    for t in range(1, n_tp):
        peer = (tp + t) % n_tp
        off = 0
        for b in range(stages):
            off = off + ((peer // (1 << b)) % 2) * (tok >> (b + 1))
        rows = pl.ds(pl.multiple_of(off, quarter), quarter)
        pltpu.make_async_remote_copy(
            src_ref=obuf.at[rows], dst_ref=obuf.at[rows],
            send_sem=agsend.at[t], recv_sem=agrecv.at[t],
            device_id={"tp": peer}, device_id_type=MESH,
        ).wait_recv()
    o_lat[...] = obuf[:, :width]
    o_krot[...] = obuf[:, width:].T[:rdim]

    @pl.loop(1, after + 1)
    def _(i):
        for c in key_copies(i):
            c.wait_send()

    @pl.loop(0, before + 1)
    def _(i):
        for s in range(stages):
            half_copy(s, i).wait_send()

        @pl.when(i > 0)
        def _():
            for c in forward_copies(i, low):
                c.wait_send()
            fin_copy(i).wait_send()

    @pl.loop(1, n_sp)
    def _(d):
        kw_copy(d).wait_send()

    for t in range(1, n_tp):
        ag_copy(t).wait_send()


def store(*refs):
    *pairs, sem = refs
    count = len(pairs) // 2
    copies = [
        pltpu.make_async_copy(pairs[n], pairs[count + n], sem.at[n]) for n in range(count)
    ]
    for c in copies:
        c.start()
    for c in copies:
        c.wait()


def per_device(mesh_dims, *args):
    n_sp, n_tp = mesh_dims
    qm, qr, lat, rot, kw, vw, ho, og, logs = args
    heads, tok = logs.shape
    width, rdim = lat.shape[1], rot.shape[1]
    args = (qm, qr, lat, rot.T, kw, vw, ho, og, logs)
    factor = (kw.shape[1] // heads + rdim) ** (-0.5)
    span = min(SEQ_DEVICES, n_sp)
    stages = n_tp.bit_length() - 1
    rpad = -(-rdim // 128) * 128
    wide = width + rpad
    quarter = tok >> stages
    part = width // n_sp
    dma = pltpu.SemaphoreType.DMA
    scratch = [pltpu.VMEM(a.shape, a.dtype) for a in args] + [
        dma((len(args),)),
        pltpu.VMEM((span, tok, width), BF16),
        pltpu.VMEM((span, rdim, tok), BF16),
        pltpu.VMEM((heads * tok, width), BF16),
        pltpu.VMEM((heads * tok, width), BF16),
        pltpu.VMEM((heads * tok, rpad), BF16),
        pltpu.VMEM((heads * tok, width), F32),
        pltpu.VMEM((heads * tok, rdim), F32),
        pltpu.VMEM((span, tok, wide), F32),
        pltpu.VMEM((tok, wide), F32),
        pltpu.VMEM((n_sp, part, kw.shape[1]), BF16),
        pltpu.VMEM((n_sp, part, kw.shape[1]), BF16),
        pltpu.VMEM((span, quarter, wide), BF16),
        pltpu.VMEM((span, quarter, wide), BF16),
        dma((span, 2)), dma((span, 2)), dma((span, 2)), dma((span, 2)),
        dma((span,)), dma((span,)), dma((n_tp,)), dma((n_tp,)), dma((n_sp,)), dma((n_sp,)),
    ]
    halves = [pltpu.VMEM((span, tok >> (s + 1), wide), BF16) for s in range(stages)]
    sems = [dma((span,)) for s in range(stages)]
    scratch = scratch + halves + halves + sems + sems
    shapes = (
        (tok, kw.shape[1]), (tok, heads * rdim), (tok, width), (rdim, tok), (part, kw.shape[1]),
    )
    results = sum(4 * math.prod(s) for s in shapes)
    vmem = pl.BlockSpec(memory_space=pltpu.VMEM)
    hbm = pl.BlockSpec(memory_space=pltpu.HBM)
    held = pl.pallas_call(
        functools.partial(kernel, (n_sp, n_tp, heads, factor)),
        out_shape=[pltpu.VMEM(s, F32) for s in shapes],
        in_specs=[hbm] * len(args),
        out_specs=[vmem] * len(shapes),
        scratch_shapes=scratch,
        compiler_params=pltpu.CompilerParams(
            collective_id=0, has_side_effects=True, vmem_limit_bytes=VMEM_BYTES - results - (16 << 10)
        ),
        name="latent_attention_backward",
    )(*args)
    main, rotary, lat_out, rot_out, weight = pl.pallas_call(
        store,
        out_shape=[jax.ShapeDtypeStruct(s, F32) for s in shapes],
        in_specs=[vmem] * len(shapes),
        out_specs=[hbm] * len(shapes),
        scratch_shapes=[dma((len(shapes),))],
        compiler_params=pltpu.CompilerParams(vmem_limit_bytes=4 << 20),
        name="store_outputs",
    )(*held)
    return main, rotary, lat_out, rot_out.T, weight


def solution(mesh):
    dims = (mesh.shape["sp"], mesh.shape["tp"])
    return jax.shard_map(
        functools.partial(per_device, dims),
        mesh=mesh,
        in_specs=(
            P("sp", "tp"),
            P("sp", "tp"),
            P("sp", None),
            P("sp", None),
            P(None, "tp"),
            P(None, "tp"),
            P("sp", "tp"),
            P("sp", "tp"),
            P("tp", "sp"),
        ),
        out_specs=(P("sp", "tp"), P("sp", "tp"), P("sp", None), P("sp", None), P("sp", "tp")),
        check_vma=False,
    )
```

```python
import functools
import math

import jax
import jax.numpy as jnp
from jax import lax
from jax.experimental import pallas as pl
from jax.experimental.pallas import tpu as pltpu
from jax.sharding import PartitionSpec as P

SEQ_DEVICES = 32
VMEM_BYTES = 67043328
MESH = pl.DeviceIdType.MESH
F32 = jnp.float32
BF16 = jnp.bfloat16


def dot(a, b, ca, cb, precision=None):
    return lax.dot_general(
        a, b, (((ca,), (cb,)), ((), ())), preferred_element_type=F32, precision=precision
    )


def kernel(
    dims,
    qm_h, qr_h, lat_h, rot_h, kw_h, vw_h, ho_h, og_h, logs_h,
    o_main, o_rot, o_lat, o_krot, o_kw,
    qm, qr, lat, rot, kw, vw, ho, og, logs, insem,
    lat_buf, rot_buf, ql, gr, qrp, mixed, rsum, gpart, obuf, kwst, kwrecv, fin_s, fin_r,
    ksend, krecv, fsend, frecv, finsend, finrecv, agsend, agrecv, kwsend, kwrecvs,
    *halving,
):
    n_sp, n_tp, heads, factor = dims
    stages = n_tp.bit_length() - 1
    half_s, half_r = halving[:stages], halving[stages : 2 * stages]
    half_ss, half_rs = halving[2 * stages : 3 * stages], halving[3 * stages :]
    span = min(SEQ_DEVICES, n_sp)
    lead = span // 4
    tok, width = lat.shape
    rdim = rot.shape[0]
    kdim = kw.shape[1] // heads
    vdim = vw.shape[1] // heads
    loads = [
        pltpu.make_async_copy(src, dst, insem.at[n])
        for n, (src, dst) in enumerate(
            (
                (lat_h, lat), (rot_h, rot), (qm_h, qm), (kw_h, kw), (og_h, og), (vw_h, vw),
                (ho_h, ho), (qr_h, qr), (logs_h, logs),
            )
        )
    ]
    for c in loads:
        c.start()
    sp = lax.axis_index("sp")
    tp = lax.axis_index("tp")
    seq = (sp + lead) // span
    first = jnp.maximum(seq * span - lead, 0)
    last = jnp.minimum((seq + 1) * span - lead, n_sp)
    before = sp - first
    after = last - 1 - sp
    low = tp % 2
    pair = tp + 1 - 2 * low

    barrier = pltpu.get_barrier_semaphore()

    @pl.loop(1, n_sp)
    def _(d):
        pl.semaphore_signal(
            barrier, inc=1, device_id={"sp": (sp + d) % n_sp}, device_id_type=MESH
        )

    for t in range(1, n_tp):
        pl.semaphore_signal(
            barrier, inc=1, device_id={"tp": (tp + t) % n_tp}, device_id_type=MESH
        )

    def part_of(side, size):
        return pl.ds(pl.multiple_of(side * (size // 2), size // 2), size // 2)

    keys = ((lat, lat_buf, tok), (rot, rot_buf, rdim))

    def key_copies(i):
        return [
            pltpu.make_async_remote_copy(
                src_ref=src.at[part_of(low, size)], dst_ref=dst.at[i, part_of(low, size)],
                send_sem=ksend.at[i, n], recv_sem=krecv.at[i, n],
                device_id={"sp": sp + i}, device_id_type=MESH,
            )
            for n, (src, dst, size) in enumerate(keys)
        ]

    def forward_copies(i, side):
        return [
            pltpu.make_async_remote_copy(
                src_ref=buf.at[i, part_of(side, size)], dst_ref=buf.at[i, part_of(side, size)],
                send_sem=fsend.at[i, n], recv_sem=frecv.at[i, n],
                device_id={"tp": pair}, device_id_type=MESH,
            )
            for n, (_, buf, size) in enumerate(keys)
        ]

    for c in loads[:4]:
        c.wait()
    lat_buf[0] = lat[...]
    rot_buf[0] = rot[...]
    for h in range(heads):
        kcols = slice(h * kdim, (h + 1) * kdim)
        ql[h * tok : (h + 1) * tok] = dot(qm[:, kcols], kw[:, kcols], 1, 1).astype(BF16)
    pl.semaphore_wait(barrier, n_sp - 1 + n_tp - 1)

    @pl.loop(1, after + 1)
    def _(i):
        for c in key_copies(i):
            c.start()

    for c in loads[4:]:
        c.wait()
    terms_parts = []
    for h in range(heads):
        rows = slice(h * tok, (h + 1) * tok)
        kcols = slice(h * kdim, (h + 1) * kdim)
        vcols = slice(h * vdim, (h + 1) * vdim)
        gr[rows] = dot(og[:, vcols], vw[:, vcols], 1, 1).astype(BF16)
        qrp[rows] = jnp.concatenate(
            [qr[:, h * rdim : (h + 1) * rdim], jnp.zeros((tok, qrp.shape[1] - rdim), BF16)], axis=1
        )
        prod = ho[:, vcols].astype(F32) * og[:, vcols].astype(F32)
        terms_parts.append(
            dot(jnp.ones((8, vdim), F32), prod, 1, 1, lax.Precision.HIGHEST)[0:1]
        )
    terms = jnp.concatenate(terms_parts, axis=1)
    row_logs = jnp.concatenate([logs[h : h + 1, :] for h in range(heads)], axis=1)

    @pl.when(before % 2 == 1)
    def _():
        lat_buf[before + 1] = jnp.zeros((tok, width), BF16)
        rot_buf[before + 1] = jnp.zeros((rdim, tok), BF16)


    def level_offset(level):
        off = 0
        for b in range(level):
            off = off + ((tp // (1 << b)) % 2) * (tok >> (b + 1))
        return off

    def half_copy(s, i):
        bit = (tp // (1 << s)) % 2
        return pltpu.make_async_remote_copy(
            src_ref=half_s[s].at[i], dst_ref=half_r[s].at[i],
            send_sem=half_ss[s].at[i], recv_sem=half_rs[s].at[i],
            device_id={"tp": tp + (1 - 2 * bit) * (1 << s)}, device_id_type=MESH,
        )

    def send_half(s, i):
        size = tok >> (s + 1)
        bit = (tp // (1 << s)) % 2
        start = pl.multiple_of(level_offset(s) + (1 - bit) * size, size)
        half_s[s][i] = gpart[i, pl.ds(start, size), :].astype(BF16)
        half_copy(s, i).start()

    def fin_copy(i):
        return pltpu.make_async_remote_copy(
            src_ref=fin_s.at[i], dst_ref=fin_r.at[i],
            send_sem=finsend.at[i], recv_sem=finrecv.at[i],
            device_id={"sp": sp - i}, device_id_type=MESH,
        )

    def arrive(i):
        for c in key_copies(i):
            c.wait_recv()
        for c in forward_copies(i, low):
            c.start()

    quarter = tok >> stages
    my_rows = pl.ds(pl.multiple_of(level_offset(stages), quarter), quarter)

    def pass_on(s, i):
        @pl.when((i >= 0) & (i <= before))
        def _():
            half_copy(s - 1, i).wait_recv()
            size = tok >> s
            rows = pl.ds(pl.multiple_of(level_offset(s), size), size)
            gpart[i, rows, :] += half_r[s - 1][i].astype(F32)
            if s < stages:
                send_half(s, i)
            else:

                @pl.when(i > 0)
                def _():
                    fin_s[i] = gpart[i, rows, :].astype(BF16)
                    fin_copy(i).start()

    def attend(i, count):
        if count:
            for b in range(count):

                @pl.when(i + b <= before)
                def _(b=b):
                    for c in forward_copies(i + b, 1 - low):
                        c.wait_recv()

        size = max(count, 1)
        lt = lat_buf[pl.ds(i, size)].reshape(size * tok, width)
        rt = jnp.concatenate([rot_buf[i + b] for b in range(size)], axis=1)
        scores = dot(lt, ql[...], 1, 1) + dot(rt, qrp[:, :rdim], 0, 1)
        weights = jnp.exp(factor * scores - row_logs)
        if not count:
            key_at = lax.broadcasted_iota(jnp.int32, weights.shape, 0)
            query_at = lax.broadcasted_iota(jnp.int32, weights.shape, 1) % tok
            weights = jnp.where(key_at <= query_at, weights, 0.0)
        slopes = dot(lt, gr[...], 1, 1)
        dscores = weights * (slopes - terms)
        wl = weights.astype(BF16)
        dl = dscores.astype(BF16)
        part_lat = factor * dot(dl, ql[...], 1, 0) + dot(wl, gr[...], 1, 0)
        part_rot = factor * dot(dl, qrp[...], 1, 0)
        gpart[pl.ds(i, size), :, :width] = part_lat.reshape(size, tok, width)
        gpart[pl.ds(i, size), :, width:] = part_rot.reshape(size, tok, part_rot.shape[1])
        for b in range(size):

            @pl.when(i + b <= before)
            def _(b=b):
                send_half(0, i + b)

        for b in range(2):

            @pl.when(i + size + b <= before)
            def _(b=b):
                arrive(i + size + b)

        if count:
            mixed[...] += dot(dl, lt, 0, 0)
            rsum[...] += dot(dl, rt, 0, 1)
        else:
            mixed[...] = dot(dl, lt, 0, 0)
            rsum[...] = dot(dl, rt, 0, 1)

    attend(0, 0)
    groups = (before + 1) // 2 + 1

    @pl.loop(1, groups + stages)
    def _(it):
        @pl.when(it < groups)
        def _():
            attend(2 * it - 1, 2)

        for s in range(1, stages + 1):
            for b in range(2):
                pass_on(s, 2 * (it - s) - 1 + b)

    part = o_kw.shape[0]

    def kw_copy(d):
        dest = (sp + d) % n_sp
        return pltpu.make_async_remote_copy(
            src_ref=kwst.at[dest], dst_ref=kwrecv.at[n_sp - d],
            send_sem=kwsend.at[d], recv_sem=kwrecvs.at[n_sp - d],
            device_id={"sp": dest}, device_id_type=MESH,
        )

    def kw_landing(d):
        return pltpu.make_async_remote_copy(
            src_ref=kwst.at[0], dst_ref=kwrecv.at[d],
            send_sem=kwsend.at[d], recv_sem=kwrecvs.at[d],
            device_id={"sp": (sp + d) % n_sp}, device_id_type=MESH,
        )

    low_parts = []
    for h in range(heads):
        rows = slice(h * tok, (h + 1) * tok)
        kcols = slice(h * kdim, (h + 1) * kdim)
        ml = mixed[rows].astype(BF16)
        term = (factor * dot(ml, qm[:, kcols], 0, 0)).astype(BF16)
        for d in range(n_sp):
            kwst[d, :, kcols] = term[d * part : (d + 1) * part]
        low_parts.append(ml)

    @pl.loop(1, n_sp)
    def _(d):
        kw_copy(d).start()

    for h in range(heads):
        rows = slice(h * tok, (h + 1) * tok)
        kcols = slice(h * kdim, (h + 1) * kdim)
        o_main[:, kcols] = factor * dot(low_parts[h], kw[:, kcols], 1, 0)
        o_rot[:, h * rdim : (h + 1) * rdim] = factor * rsum[rows]

    @pl.loop(1, after + 1)
    def _(i):
        pltpu.make_async_remote_copy(
            src_ref=fin_s.at[i], dst_ref=fin_r.at[i],
            send_sem=finsend.at[i], recv_sem=finrecv.at[i],
            device_id={"sp": sp + i}, device_id_type=MESH,
        ).wait_recv()
        gpart[0, my_rows, :] += fin_r[i].astype(F32)

    obuf[my_rows] = gpart[0, my_rows, :]

    def ag_copy(t):
        return pltpu.make_async_remote_copy(
            src_ref=obuf.at[my_rows], dst_ref=obuf.at[my_rows],
            send_sem=agsend.at[t], recv_sem=agrecv.at[n_tp - t],
            device_id={"tp": (tp + t) % n_tp}, device_id_type=MESH,
        )

    for t in range(1, n_tp):
        ag_copy(t).start()

    total = kwst[sp].astype(F32)
    for d in range(1, n_sp):
        kw_landing(d).wait_recv()
        total = total + kwrecv[d].astype(F32)
    o_kw[...] = total

    for t in range(1, n_tp):
        peer = (tp + t) % n_tp
        off = 0
        for b in range(stages):
            off = off + ((peer // (1 << b)) % 2) * (tok >> (b + 1))
        rows = pl.ds(pl.multiple_of(off, quarter), quarter)
        pltpu.make_async_remote_copy(
            src_ref=obuf.at[rows], dst_ref=obuf.at[rows],
            send_sem=agsend.at[t], recv_sem=agrecv.at[t],
            device_id={"tp": peer}, device_id_type=MESH,
        ).wait_recv()
    o_lat[...] = obuf[:, :width]
    o_krot[...] = obuf[:, width:].T[:rdim]

    @pl.loop(1, after + 1)
    def _(i):
        for c in key_copies(i):
            c.wait_send()

    @pl.loop(0, before + 1)
    def _(i):
        for s in range(stages):
            half_copy(s, i).wait_send()

        @pl.when(i > 0)
        def _():
            for c in forward_copies(i, low):
                c.wait_send()
            fin_copy(i).wait_send()

    @pl.loop(1, n_sp)
    def _(d):
        kw_copy(d).wait_send()

    for t in range(1, n_tp):
        ag_copy(t).wait_send()


def store(*refs):
    *pairs, sem = refs
    count = len(pairs) // 2
    copies = [
        pltpu.make_async_copy(pairs[n], pairs[count + n], sem.at[n]) for n in range(count)
    ]
    for c in copies:
        c.start()
    for c in copies:
        c.wait()


def per_device(mesh_dims, *args):
    n_sp, n_tp = mesh_dims
    qm, qr, lat, rot, kw, vw, ho, og, logs = args
    heads, tok = logs.shape
    width, rdim = lat.shape[1], rot.shape[1]
    args = (qm, qr, lat, rot.T, kw, vw, ho, og, logs)
    factor = (kw.shape[1] // heads + rdim) ** (-0.5)
    span = min(SEQ_DEVICES, n_sp)
    stages = n_tp.bit_length() - 1
    rpad = -(-rdim // 128) * 128
    wide = width + rpad
    quarter = tok >> stages
    part = width // n_sp
    dma = pltpu.SemaphoreType.DMA
    scratch = [pltpu.VMEM(a.shape, a.dtype) for a in args] + [
        dma((len(args),)),
        pltpu.VMEM((span + 1, tok, width), BF16),
        pltpu.VMEM((span + 1, rdim, tok), BF16),
        pltpu.VMEM((heads * tok, width), BF16),
        pltpu.VMEM((heads * tok, width), BF16),
        pltpu.VMEM((heads * tok, rpad), BF16),
        pltpu.VMEM((heads * tok, width), F32),
        pltpu.VMEM((heads * tok, rdim), F32),
        pltpu.VMEM((span + 1, tok, wide), F32),
        pltpu.VMEM((tok, wide), F32),
        pltpu.VMEM((n_sp, part, kw.shape[1]), BF16),
        pltpu.VMEM((n_sp, part, kw.shape[1]), BF16),
        pltpu.VMEM((span, quarter, wide), BF16),
        pltpu.VMEM((span, quarter, wide), BF16),
        dma((span, 2)), dma((span, 2)), dma((span, 2)), dma((span, 2)),
        dma((span,)), dma((span,)), dma((n_tp,)), dma((n_tp,)), dma((n_sp,)), dma((n_sp,)),
    ]
    halves = [pltpu.VMEM((span, tok >> (s + 1), wide), BF16) for s in range(stages)]
    sems = [dma((span,)) for s in range(stages)]
    scratch = scratch + halves + halves + sems + sems
    shapes = (
        (tok, kw.shape[1]), (tok, heads * rdim), (tok, width), (rdim, tok), (part, kw.shape[1]),
    )
    results = sum(4 * math.prod(s) for s in shapes)
    vmem = pl.BlockSpec(memory_space=pltpu.VMEM)
    hbm = pl.BlockSpec(memory_space=pltpu.HBM)
    held = pl.pallas_call(
        functools.partial(kernel, (n_sp, n_tp, heads, factor)),
        out_shape=[pltpu.VMEM(s, F32) for s in shapes],
        in_specs=[hbm] * len(args),
        out_specs=[vmem] * len(shapes),
        scratch_shapes=scratch,
        compiler_params=pltpu.CompilerParams(
            collective_id=0, has_side_effects=True, vmem_limit_bytes=VMEM_BYTES - results - (16 << 10)
        ),
        name="latent_attention_backward",
    )(*args)
    main, rotary, lat_out, rot_out, weight = pl.pallas_call(
        store,
        out_shape=[jax.ShapeDtypeStruct(s, F32) for s in shapes],
        in_specs=[vmem] * len(shapes),
        out_specs=[hbm] * len(shapes),
        scratch_shapes=[dma((len(shapes),))],
        compiler_params=pltpu.CompilerParams(vmem_limit_bytes=4 << 20),
        name="store_outputs",
    )(*held)
    return main, rotary, lat_out, rot_out.T, weight


def solution(mesh):
    dims = (mesh.shape["sp"], mesh.shape["tp"])
    return jax.shard_map(
        functools.partial(per_device, dims),
        mesh=mesh,
        in_specs=(
            P("sp", "tp"),
            P("sp", "tp"),
            P("sp", None),
            P("sp", None),
            P(None, "tp"),
            P(None, "tp"),
            P("sp", "tp"),
            P("sp", "tp"),
            P("tp", "sp"),
        ),
        out_specs=(P("sp", "tp"), P("sp", "tp"), P("sp", None), P("sp", None), P("sp", "tp")),
        check_vma=False,
    )
```

```python
import functools
import math

import jax
import jax.numpy as jnp
from jax import lax
from jax.experimental import pallas as pl
from jax.experimental.pallas import tpu as pltpu
from jax.sharding import PartitionSpec as P

SEQ_DEVICES = 32
VMEM_BYTES = 67043328
MESH = pl.DeviceIdType.MESH
F32 = jnp.float32
BF16 = jnp.bfloat16


def dot(a, b, ca, cb, precision=None):
    return lax.dot_general(
        a, b, (((ca,), (cb,)), ((), ())), preferred_element_type=F32, precision=precision
    )


def kernel(
    dims,
    qm_h, qr_h, lat_h, rot_h, kw_h, vw_h, ho_h, og_h, logs_h,
    o_main, o_rot, o_lat, o_krot, o_kw,
    qm, qr, lat, rot, kw, vw, ho, og, logs, insem,
    lat_buf, rot_buf, ql, gr, qrp, mixed, rsum, gpart, obuf, kwst, kwrecv, fin_s, fin_r,
    ksend, krecv, fsend, frecv, finsend, finrecv, agsend, agrecv, kwsend, kwrecvs,
    *halving,
):
    n_sp, n_tp, heads, factor = dims
    stages = n_tp.bit_length() - 1
    half_s, half_r = halving[:stages], halving[stages : 2 * stages]
    half_ss, half_rs = halving[2 * stages : 3 * stages], halving[3 * stages :]
    span = min(SEQ_DEVICES, n_sp)
    lead = span // 4
    tok, width = lat.shape
    rdim = rot.shape[0]
    kdim = kw.shape[1] // heads
    vdim = vw.shape[1] // heads
    loads = [
        pltpu.make_async_copy(src, dst, insem.at[n])
        for n, (src, dst) in enumerate(
            (
                (lat_h, lat), (rot_h, rot), (qm_h, qm), (kw_h, kw), (og_h, og), (vw_h, vw),
                (ho_h, ho), (qr_h, qr), (logs_h, logs),
            )
        )
    ]
    for c in loads:
        c.start()
    sp = lax.axis_index("sp")
    tp = lax.axis_index("tp")
    seq = (sp + lead) // span
    first = jnp.maximum(seq * span - lead, 0)
    last = jnp.minimum((seq + 1) * span - lead, n_sp)
    before = sp - first
    after = last - 1 - sp
    low = tp % 2
    pair = tp + 1 - 2 * low

    barrier = pltpu.get_barrier_semaphore()

    @pl.loop(1, n_sp)
    def _(d):
        pl.semaphore_signal(
            barrier, inc=1, device_id={"sp": (sp + d) % n_sp}, device_id_type=MESH
        )

    for t in range(1, n_tp):
        pl.semaphore_signal(
            barrier, inc=1, device_id={"tp": (tp + t) % n_tp}, device_id_type=MESH
        )

    def part_of(side, size):
        return pl.ds(pl.multiple_of(side * (size // 2), size // 2), size // 2)

    keys = ((lat, lat_buf, tok), (rot, rot_buf, rdim))

    def key_copies(i):
        return [
            pltpu.make_async_remote_copy(
                src_ref=src.at[part_of(low, size)], dst_ref=dst.at[i, part_of(low, size)],
                send_sem=ksend.at[i, n], recv_sem=krecv.at[i, n],
                device_id={"sp": sp + i}, device_id_type=MESH,
            )
            for n, (src, dst, size) in enumerate(keys)
        ]

    def forward_copies(i, side):
        return [
            pltpu.make_async_remote_copy(
                src_ref=buf.at[i, part_of(side, size)], dst_ref=buf.at[i, part_of(side, size)],
                send_sem=fsend.at[i, n], recv_sem=frecv.at[i, n],
                device_id={"tp": pair}, device_id_type=MESH,
            )
            for n, (_, buf, size) in enumerate(keys)
        ]

    for c in loads[:4]:
        c.wait()
    lat_buf[0] = lat[...]
    rot_buf[0] = rot[...]
    for h in range(heads):
        kcols = slice(h * kdim, (h + 1) * kdim)
        ql[h * tok : (h + 1) * tok] = dot(qm[:, kcols], kw[:, kcols], 1, 1).astype(BF16)
    pl.semaphore_wait(barrier, n_sp - 1 + n_tp - 1)

    @pl.loop(1, after + 1)
    def _(i):
        for c in key_copies(i):
            c.start()

    for c in loads[4:]:
        c.wait()
    terms_parts = []
    for h in range(heads):
        rows = slice(h * tok, (h + 1) * tok)
        kcols = slice(h * kdim, (h + 1) * kdim)
        vcols = slice(h * vdim, (h + 1) * vdim)
        gr[rows] = dot(og[:, vcols], vw[:, vcols], 1, 1).astype(BF16)
        qrp[rows] = jnp.concatenate(
            [qr[:, h * rdim : (h + 1) * rdim], jnp.zeros((tok, qrp.shape[1] - rdim), BF16)], axis=1
        )
        prod = ho[:, vcols].astype(F32) * og[:, vcols].astype(F32)
        terms_parts.append(
            dot(jnp.ones((8, vdim), F32), prod, 1, 1, lax.Precision.HIGHEST)[0:1]
        )
    terms = jnp.concatenate(terms_parts, axis=1)
    row_logs = jnp.concatenate([logs[h : h + 1, :] for h in range(heads)], axis=1)

    @pl.when(before % 2 == 1)
    def _():
        lat_buf[before + 1] = jnp.zeros((tok, width), BF16)
        rot_buf[before + 1] = jnp.zeros((rdim, tok), BF16)


    def level_offset(level):
        off = 0
        for b in range(level):
            off = off + ((tp // (1 << b)) % 2) * (tok >> (b + 1))
        return off

    def half_copy(s, i):
        bit = (tp // (1 << s)) % 2
        return pltpu.make_async_remote_copy(
            src_ref=half_s[s].at[i], dst_ref=half_r[s].at[i],
            send_sem=half_ss[s].at[i], recv_sem=half_rs[s].at[i],
            device_id={"tp": tp + (1 - 2 * bit) * (1 << s)}, device_id_type=MESH,
        )

    def send_half(s, i):
        size = tok >> (s + 1)
        bit = (tp // (1 << s)) % 2
        start = pl.multiple_of(level_offset(s) + (1 - bit) * size, size)
        half_s[s][i] = gpart[i, pl.ds(start, size), :].astype(half_s[s].dtype)
        half_copy(s, i).start()

    def fin_copy(i):
        return pltpu.make_async_remote_copy(
            src_ref=fin_s.at[i], dst_ref=fin_r.at[i],
            send_sem=finsend.at[i], recv_sem=finrecv.at[i],
            device_id={"sp": sp - i}, device_id_type=MESH,
        )

    def arrive(i):
        for c in key_copies(i):
            c.wait_recv()
        for c in forward_copies(i, low):
            c.start()

    quarter = tok >> stages
    my_rows = pl.ds(pl.multiple_of(level_offset(stages), quarter), quarter)

    def pass_on(s, i):
        @pl.when((i >= 0) & (i <= before))
        def _():
            half_copy(s - 1, i).wait_recv()
            size = tok >> s
            rows = pl.ds(pl.multiple_of(level_offset(s), size), size)
            gpart[i, rows, :] += half_r[s - 1][i].astype(F32)
            if s < stages:
                send_half(s, i)
            else:

                @pl.when(i > 0)
                def _():
                    fin_s[i] = gpart[i, rows, :].astype(BF16)
                    fin_copy(i).start()

    def attend(i, count):
        if count:
            for b in range(count):

                @pl.when(i + b <= before)
                def _(b=b):
                    for c in forward_copies(i + b, 1 - low):
                        c.wait_recv()

        size = max(count, 1)
        lt = lat_buf[pl.ds(i, size)].reshape(size * tok, width)
        rt = jnp.concatenate([rot_buf[i + b] for b in range(size)], axis=1)
        scores = dot(lt, ql[...], 1, 1) + dot(rt, qrp[:, :rdim], 0, 1)
        weights = jnp.exp(factor * scores - row_logs)
        if not count:
            key_at = lax.broadcasted_iota(jnp.int32, weights.shape, 0)
            query_at = lax.broadcasted_iota(jnp.int32, weights.shape, 1) % tok
            weights = jnp.where(key_at <= query_at, weights, 0.0)
        slopes = dot(lt, gr[...], 1, 1)
        dscores = weights * (slopes - terms)
        wl = weights.astype(BF16)
        dl = dscores.astype(BF16)
        part_lat = factor * dot(dl, ql[...], 1, 0) + dot(wl, gr[...], 1, 0)
        part_rot = factor * dot(dl, qrp[...], 1, 0)
        gpart[pl.ds(i, size), :, :width] = part_lat.reshape(size, tok, width)
        gpart[pl.ds(i, size), :, width:] = part_rot.reshape(size, tok, part_rot.shape[1])
        for b in range(size):

            @pl.when(i + b <= before)
            def _(b=b):
                send_half(0, i + b)

        for b in range(2):

            @pl.when(i + size + b <= before)
            def _(b=b):
                arrive(i + size + b)

        if count:
            mixed[...] += dot(dl, lt, 0, 0)
            rsum[...] += dot(dl, rt, 0, 1)
        else:
            mixed[...] = dot(dl, lt, 0, 0)
            rsum[...] = dot(dl, rt, 0, 1)

    attend(0, 0)
    groups = (before + 1) // 2 + 1

    @pl.loop(1, groups + stages)
    def _(it):
        for s in range(1, stages + 1):
            for b in range(2):
                pass_on(s, 2 * (it - s) - 1 + b)

        @pl.when(it < groups)
        def _():
            attend(2 * it - 1, 2)

    part = o_kw.shape[0]

    def kw_copy(d):
        dest = (sp + d) % n_sp
        return pltpu.make_async_remote_copy(
            src_ref=kwst.at[dest], dst_ref=kwrecv.at[n_sp - d],
            send_sem=kwsend.at[d], recv_sem=kwrecvs.at[n_sp - d],
            device_id={"sp": dest}, device_id_type=MESH,
        )

    def kw_landing(d):
        return pltpu.make_async_remote_copy(
            src_ref=kwst.at[0], dst_ref=kwrecv.at[d],
            send_sem=kwsend.at[d], recv_sem=kwrecvs.at[d],
            device_id={"sp": (sp + d) % n_sp}, device_id_type=MESH,
        )

    low_parts = []
    for h in range(heads):
        rows = slice(h * tok, (h + 1) * tok)
        kcols = slice(h * kdim, (h + 1) * kdim)
        ml = mixed[rows].astype(BF16)
        term = (factor * dot(ml, qm[:, kcols], 0, 0)).astype(BF16)
        for d in range(n_sp):
            kwst[d, :, kcols] = term[d * part : (d + 1) * part]
        low_parts.append(ml)

    @pl.loop(1, n_sp)
    def _(d):
        kw_copy(d).start()

    for h in range(heads):
        rows = slice(h * tok, (h + 1) * tok)
        kcols = slice(h * kdim, (h + 1) * kdim)
        o_main[:, kcols] = factor * dot(low_parts[h], kw[:, kcols], 1, 0)
        o_rot[:, h * rdim : (h + 1) * rdim] = factor * rsum[rows]

    @pl.loop(1, after + 1)
    def _(i):
        pltpu.make_async_remote_copy(
            src_ref=fin_s.at[i], dst_ref=fin_r.at[i],
            send_sem=finsend.at[i], recv_sem=finrecv.at[i],
            device_id={"sp": sp + i}, device_id_type=MESH,
        ).wait_recv()
        gpart[0, my_rows, :] += fin_r[i].astype(F32)

    obuf[my_rows] = gpart[0, my_rows, :].astype(BF16)

    def ag_copy(t):
        return pltpu.make_async_remote_copy(
            src_ref=obuf.at[my_rows], dst_ref=obuf.at[my_rows],
            send_sem=agsend.at[t], recv_sem=agrecv.at[n_tp - t],
            device_id={"tp": (tp + t) % n_tp}, device_id_type=MESH,
        )

    for t in range(1, n_tp):
        ag_copy(t).start()

    total = kwst[sp].astype(F32)
    for d in range(1, n_sp):
        kw_landing(d).wait_recv()
        total = total + kwrecv[d].astype(F32)
    o_kw[...] = total

    for t in range(1, n_tp):
        peer = (tp + t) % n_tp
        off = 0
        for b in range(stages):
            off = off + ((peer // (1 << b)) % 2) * (tok >> (b + 1))
        rows = pl.ds(pl.multiple_of(off, quarter), quarter)
        pltpu.make_async_remote_copy(
            src_ref=obuf.at[rows], dst_ref=obuf.at[rows],
            send_sem=agsend.at[t], recv_sem=agrecv.at[t],
            device_id={"tp": peer}, device_id_type=MESH,
        ).wait_recv()
    o_lat[...] = obuf[:, :width].astype(F32)
    o_krot[...] = obuf[:, width:].astype(F32).T[:rdim]

    @pl.loop(1, after + 1)
    def _(i):
        for c in key_copies(i):
            c.wait_send()

    @pl.loop(0, before + 1)
    def _(i):
        for s in range(stages):
            half_copy(s, i).wait_send()

        @pl.when(i > 0)
        def _():
            for c in forward_copies(i, low):
                c.wait_send()
            fin_copy(i).wait_send()

    @pl.loop(1, n_sp)
    def _(d):
        kw_copy(d).wait_send()

    for t in range(1, n_tp):
        ag_copy(t).wait_send()


def store(*refs):
    *pairs, sem = refs
    count = len(pairs) // 2
    copies = [
        pltpu.make_async_copy(pairs[n], pairs[count + n], sem.at[n]) for n in range(count)
    ]
    for c in copies:
        c.start()
    for c in copies:
        c.wait()


def per_device(mesh_dims, *args):
    n_sp, n_tp = mesh_dims
    qm, qr, lat, rot, kw, vw, ho, og, logs = args
    heads, tok = logs.shape
    width, rdim = lat.shape[1], rot.shape[1]
    args = (qm, qr, lat, rot.T, kw, vw, ho, og, logs)
    factor = (kw.shape[1] // heads + rdim) ** (-0.5)
    span = min(SEQ_DEVICES, n_sp)
    stages = n_tp.bit_length() - 1
    rpad = -(-rdim // 128) * 128
    wide = width + rpad
    quarter = tok >> stages
    part = width // n_sp
    dma = pltpu.SemaphoreType.DMA
    scratch = [pltpu.VMEM(a.shape, a.dtype) for a in args] + [
        dma((len(args),)),
        pltpu.VMEM((span + 1, tok, width), BF16),
        pltpu.VMEM((span + 1, rdim, tok), BF16),
        pltpu.VMEM((heads * tok, width), BF16),
        pltpu.VMEM((heads * tok, width), BF16),
        pltpu.VMEM((heads * tok, rpad), BF16),
        pltpu.VMEM((heads * tok, width), F32),
        pltpu.VMEM((heads * tok, rdim), F32),
        pltpu.VMEM((span + 1, tok, wide), F32),
        pltpu.VMEM((tok, wide), BF16),
        pltpu.VMEM((n_sp, part, kw.shape[1]), BF16),
        pltpu.VMEM((n_sp, part, kw.shape[1]), BF16),
        pltpu.VMEM((span, quarter, wide), BF16),
        pltpu.VMEM((span, quarter, wide), BF16),
        dma((span, 2)), dma((span, 2)), dma((span, 2)), dma((span, 2)),
        dma((span,)), dma((span,)), dma((n_tp,)), dma((n_tp,)), dma((n_sp,)), dma((n_sp,)),
    ]
    halves = [
        pltpu.VMEM((span, tok >> (s + 1), wide), BF16 if s else F32) for s in range(stages)
    ]
    sems = [dma((span,)) for s in range(stages)]
    scratch = scratch + halves + halves + sems + sems
    shapes = (
        (tok, kw.shape[1]), (tok, heads * rdim), (tok, width), (rdim, tok), (part, kw.shape[1]),
    )
    results = sum(4 * math.prod(s) for s in shapes)
    vmem = pl.BlockSpec(memory_space=pltpu.VMEM)
    hbm = pl.BlockSpec(memory_space=pltpu.HBM)
    held = pl.pallas_call(
        functools.partial(kernel, (n_sp, n_tp, heads, factor)),
        out_shape=[pltpu.VMEM(s, F32) for s in shapes],
        in_specs=[hbm] * len(args),
        out_specs=[vmem] * len(shapes),
        scratch_shapes=scratch,
        compiler_params=pltpu.CompilerParams(
            collective_id=0, has_side_effects=True, vmem_limit_bytes=VMEM_BYTES - results - (16 << 10)
        ),
        name="latent_attention_backward",
    )(*args)
    main, rotary, lat_out, rot_out, weight = pl.pallas_call(
        store,
        out_shape=[jax.ShapeDtypeStruct(s, F32) for s in shapes],
        in_specs=[vmem] * len(shapes),
        out_specs=[hbm] * len(shapes),
        scratch_shapes=[dma((len(shapes),))],
        compiler_params=pltpu.CompilerParams(vmem_limit_bytes=4 << 20),
        name="store_outputs",
    )(*held)
    return main, rotary, lat_out, rot_out.T, weight


def solution(mesh):
    dims = (mesh.shape["sp"], mesh.shape["tp"])
    return jax.shard_map(
        functools.partial(per_device, dims),
        mesh=mesh,
        in_specs=(
            P("sp", "tp"),
            P("sp", "tp"),
            P("sp", None),
            P("sp", None),
            P(None, "tp"),
            P(None, "tp"),
            P("sp", "tp"),
            P("sp", "tp"),
            P("tp", "sp"),
        ),
        out_specs=(P("sp", "tp"), P("sp", "tp"), P("sp", None), P("sp", None), P("sp", "tp")),
        check_vma=False,
    )
```
